32 devices in a mesh: rep: 4 (over y, x), fs: 2 (over core), tp: 4 (over z).
Axes of the slice: x: 2, y: 2, z: 4, core: 2. Of those that a mesh axis runs over, the one named last changes fastest.
Arguments:
- layer_input: bfloat16 [10240, 2048], P(('rep', 'fs'), 'tp'), may hold values from -6 to 6
- cotangent: bfloat16 [10240, 2048], P(('rep', 'fs'), 'tp'), may hold values from -8 to 8
- gate_pre: bfloat16 [10240, 3072], P('rep', 'fs'), may hold values from -8 to 8
- up_pre: bfloat16 [10240, 3072], P('rep', 'fs'), may hold values from -6 to 6
- gate_weight: bfloat16 [2048, 3072], P('tp', 'fs'), may hold values from -0.125 to 0.125
- up_weight: bfloat16 [2048, 3072], P('tp', 'fs'), may hold values from -0.125 to 0.125
- down_weight: bfloat16 [3072, 2048], P('fs', 'tp'), may hold values from -0.109375 to 0.109375
Outputs:
- input_grad: bfloat16 [10240, 2048], P(('rep', 'fs'), 'tp')
- gate_grad: float32 [2048, 3072], P('tp', 'fs')
- up_grad: float32 [2048, 3072], P('tp', 'fs')
- down_grad: float32 [3072, 2048], P('fs', 'tp')
- gate_rows_sq: float32 [2048], P('tp')
- up_rows_sq: float32 [2048], P('tp')
- down_rows_sq: float32 [3072], P('fs')
The draws below stay inside these ranges and needn't reach their ends.
All inputs are finite; a program needn't handle non-finite values.
Results may differ from the reference program's by a relative error of at most 0.019.
Values may be sent and summed in bfloat16 or wider, within the bound.
No kernel may reach another device: no remote copies, remote signals or barrier semaphores. Data moves between devices by JAX's collectives and lax.ppermute only.
A program may use at most 128 MiB of HBM per device.

```python
import math
import jax
import jax.numpy as jnp
from jax import lax

D = 2048
FF = 3072
TOKENS = 10240
N_FS = 2


def with_spikes(values, own_key, source, target, blocks, factor):
    owner, partner = [(jnp.arange(values.shape[position]) // (values.shape[position] // blocks)).reshape([-1 if axis == position else 1 for axis in range(values.ndim)]) for position in (source, target)]
    chosen = jax.random.permutation(own_key, blocks)[partner]
    strong = (owner == chosen) | (owner == (partner + blocks // 2) % blocks)
    return jnp.where(strong, factor * values, values)


def steps_of(key, shape, pieces, smallest, top_value):
    loudness, own = 1.0, jax.random.fold_in(key, 6)
    for dim, blocks in pieces:
        heights = jnp.exp(jax.random.uniform(jax.random.fold_in(own, dim), (blocks,), jnp.float32, smallest / len(pieces), top_value / len(pieces)))
        loudness = loudness * jnp.repeat(heights, shape[dim] // blocks).reshape([-1 if axis == dim else 1 for axis in range(len(shape))])
    return loudness


def bell_draw(key, shape, deviation, most, shards=(), held_as=jnp.bfloat16):
    drawn = deviation * jax.random.normal(key, shape, jnp.float32)
    if shards:
        drawn = drawn * steps_of(key, shape, shards, -0.22, 0.18)
    return jnp.clip(drawn, -most, most).astype(held_as)


def heavy_noise(stream_key, extent, spread, limit, shards, heavy, kind=jnp.bfloat16):
    drawn = spread * jax.random.normal(stream_key, extent, jnp.float32)
    if shards:
        drawn = drawn * steps_of(stream_key, extent, shards, -0.22, 0.18)
    return jnp.clip(with_spikes(drawn, jax.random.fold_in(stream_key, 3), *heavy), -limit, limit).astype(kind)


def setup_inputs(seed: int = 0) -> dict:
    seeds = jax.random.split(jax.random.key(seed), 8)
    return {
        "layer_input": bell_draw(seeds[0], (TOKENS, D), 1.0, 6.0, ((0, 8), (1, 4))),
        "cotangent": heavy_noise(seeds[1], (TOKENS, D), 1.0, 8.0, ((0, 8), (1, 4)), (0, 1, 8, 2.0)),
        "gate_pre": bell_draw(seeds[2], (TOKENS, FF), 1.5, 8.0, ((0, 4), (1, 2))),
        "up_pre": bell_draw(seeds[3], (TOKENS, FF), 1.0, 6.0, ((0, 4), (1, 2))),
        "gate_weight": bell_draw(seeds[4], (D, FF), D ** -0.5, 0.125, ((0, 4), (1, 2))),
        "up_weight": bell_draw(seeds[5], (D, FF), D ** -0.5, 0.125, ((0, 4), (1, 2))),
        "down_weight": bell_draw(seeds[6], (FF, D), FF ** -0.5, 0.109375, ((0, 2), (1, 4))),
    }


def contract_rows(left_side, right_side):
    return lax.dot_general(left_side, right_side, (((0,), (0,)), ((), ())), preferred_element_type=jnp.float32)

def contract_cols(left_side, right_side):
    return lax.dot_general(left_side, right_side, (((1,), (1,)), ((), ())), preferred_element_type=jnp.float32)

def reference(layer_input, cotangent, gate_pre, up_pre, gate_weight, up_weight, down_weight):
    hidden_grad = contract_cols(cotangent, down_weight)
    gate_value = gate_pre.astype(jnp.float32)
    up_value = up_pre.astype(jnp.float32)
    sigmoid_gate = jax.nn.sigmoid(gate_value)
    activated = gate_value * sigmoid_gate
    hidden = (activated * up_value).astype(jnp.bfloat16)
    gate_delta = (hidden_grad * up_value * sigmoid_gate * (1.0 + gate_value * (1.0 - sigmoid_gate))).astype(jnp.bfloat16)
    up_delta = (hidden_grad * activated).astype(jnp.bfloat16)
    block = FF // N_FS
    input_sum = jnp.zeros((TOKENS, D), jnp.float32)
    for block_index in range(N_FS):
        first = block_index * block
        partial_sum = contract_cols(gate_delta[:, first:first + block], gate_weight[:, first:first + block])
        partial_sum = partial_sum + contract_cols(up_delta[:, first:first + block], up_weight[:, first:first + block])
        rounded = lax.optimization_barrier(partial_sum.astype(jnp.bfloat16))
        input_sum = input_sum + rounded.astype(jnp.float32)
    input_grad = input_sum.astype(jnp.bfloat16)
    grad_scale = 1.0 / math.sqrt(TOKENS)
    gate_grad = contract_rows(layer_input, gate_delta) * grad_scale
    up_grad = contract_rows(layer_input, up_delta) * grad_scale
    down_grad = contract_rows(hidden, cotangent) * grad_scale
    gate_rows_sq = lax.optimization_barrier(jnp.sum(gate_grad * gate_grad, axis=1))
    up_rows_sq = lax.optimization_barrier(jnp.sum(up_grad * up_grad, axis=1))
    down_rows_sq = lax.optimization_barrier(jnp.sum(down_grad * down_grad, axis=1))
    return (input_grad, gate_grad, up_grad, down_grad, gate_rows_sq, up_rows_sq, down_rows_sq)
```

```python
import functools
import math

import jax
import jax.numpy as jnp
from jax import lax
from jax.experimental import pallas as pl
from jax.experimental.pallas import tpu as pltpu
from jax.sharding import PartitionSpec as P

F32 = jnp.float32
BF16 = jnp.bfloat16
TOKEN_CHUNKS = 4


def dot(left, right, left_dim, right_dim):
    return lax.dot_general(
        left, right, (((left_dim,), (right_dim,)), ((), ())), preferred_element_type=F32
    )


def swap(value, axis, size, mask):
    return lax.ppermute(value, axis, [(i, i ^ mask) for i in range(size)])


def rotate(value, axis, size, shift):
    return lax.ppermute(value, axis, [(i, (i - shift) % size) for i in range(size)])


def down_kernel(scale, order_ref, *refs):
    *token_refs, gate_ref, up_ref, out_ref, acc_ref = refs
    part, step = pl.program_id(0), pl.program_id(1)

    @pl.when((part == 0) & (step == 0))
    def _():
        acc_ref[...] = jnp.zeros_like(acc_ref)

    gate = gate_ref[...].astype(F32)
    hidden = (gate * jax.nn.sigmoid(gate) * up_ref[...].astype(F32)).astype(BF16)
    for index, ref in enumerate(token_refs):

        @pl.when(part == index)
        def _(ref=ref):
            acc_ref[...] += dot(hidden, ref[...], 0, 0)

    @pl.when((part == len(token_refs) - 1) & (step == pl.num_programs(1) - 1))
    def _():
        out_ref[...] = acc_ref[...] * scale


def down_partial(order, parts, gate_pre, up_pre, scale, tile):
    tokens, width = parts[0].shape
    hidden = gate_pre.shape[1]
    steps = tokens // tile

    def part_spec(index):
        def place(part, step, order_ref):
            at = jnp.where(part == index, step, jnp.where(part < index, 0, steps - 1))
            return (at, 0)

        return pl.BlockSpec((tile, width), place)

    rows = pl.BlockSpec(
        (tile, hidden), lambda part, step, order_ref: (order_ref[part] * steps + step, 0)
    )
    return pl.pallas_call(
        functools.partial(down_kernel, scale),
        grid_spec=pltpu.PrefetchScalarGridSpec(
            num_scalar_prefetch=1,
            grid=(len(parts), steps),
            in_specs=[part_spec(index) for index in range(len(parts))] + [rows, rows],
            out_specs=pl.BlockSpec(
                (hidden, width), lambda part, step, order_ref: (0, 0),
                pipeline_mode=pl.Buffered(1),
            ),
            scratch_shapes=[pltpu.VMEM((hidden, width), F32)],
        ),
        out_shape=jax.ShapeDtypeStruct((hidden, width), F32),
        name="down_partial",
    )(order, *parts, gate_pre, up_pre)


def chunk_kernel(n_parts, n_blocks, scale, order_ref, block_ref, chunk_ref, *refs):
    refs = list(refs)
    cot_ref = refs.pop(0)
    weight_refs = [refs.pop(0) for _ in range(n_blocks - 1)]
    far_refs = [refs.pop(0) for _ in range(2)]
    token_refs = [refs.pop(0) for _ in range(n_parts)]
    gate_ref, up_ref, gate_w_ref, up_w_ref = [refs.pop(0) for _ in range(4)]
    gate_in_ref, up_in_ref, input_ref, gate_out_ref, up_out_ref = refs
    part, step = pl.program_id(0), pl.program_id(1)

    @pl.when((part == 0) & (step == 0))
    def _():
        gate_out_ref[...] = gate_in_ref[...]
        up_out_ref[...] = up_in_ref[...]

    n_tp = cot_ref.shape[0]
    width = weight_refs[0].shape[1]
    token = token_refs[0][...]
    for index in range(1, n_parts):
        token = jnp.where(part == index, token_refs[index][...], token)
    total = None
    for block in range(n_blocks):
        columns = pl.ds(pl.multiple_of(block_ref[block] * width, width), width)
        hidden_grad = None
        for t in range(n_tp):
            if block < n_blocks - 1:
                weight = weight_refs[block][t]
            else:
                half = n_tp // 2
                weight = far_refs[t // half][t % half]
            term = dot(cot_ref[t, 0], weight, 1, 1)
            hidden_grad = term if hidden_grad is None else hidden_grad + term
        gate = gate_ref[:, columns].astype(F32)
        up = up_ref[:, columns].astype(F32)
        sigmoid = jax.nn.sigmoid(gate)
        gate_delta = (hidden_grad * up * sigmoid * (1.0 + gate * (1.0 - sigmoid))).astype(BF16)
        up_delta = (hidden_grad * (gate * sigmoid)).astype(BF16)
        gate_out_ref[:, columns] += dot(token, gate_delta, 0, 0)
        up_out_ref[:, columns] += dot(token, up_delta, 0, 0)
        term = dot(gate_delta, gate_w_ref[:, columns], 1, 1)
        term = term + dot(up_delta, up_w_ref[:, columns], 1, 1)
        total = term if total is None else total + term
    input_ref[0] = total.astype(BF16)

    done = (part == n_parts - 1) & (step == pl.num_programs(1) - 1)

    @pl.when(done & (chunk_ref[1] == 1))
    def _():
        gate_out_ref[...] = gate_out_ref[...] * scale
        up_out_ref[...] = up_out_ref[...] * scale


def chunk_grads(
    order, blocks, cot, weights, far, tokens, gate_pre, up_pre, gate_w, up_w, sums,
    place, scale, tile,
):
    n_tp, n_fs, rows, features = cot.shape
    all_rows = gate_pre.shape[0] // n_fs
    hidden = gate_pre.shape[1]
    steps = rows // tile
    whole = pl.Buffered(1)

    def fixed(shape):
        return pl.BlockSpec(shape, lambda *_: (0,) * len(shape), pipeline_mode=whole)

    def token_spec(index):
        def place(part, step, order_ref, block_ref, chunk_ref):
            at = jnp.where(part == index, step, jnp.where(part < index, 0, steps - 1))
            return (chunk_ref[0] * steps + at, 0)

        return pl.BlockSpec((tile, features), place)

    pre = pl.BlockSpec(
        (tile, hidden),
        lambda part, step, order_ref, block_ref, chunk_ref: (
            order_ref[part] * (all_rows // tile) + chunk_ref[0] * steps + step, 0,
        ),
    )
    in_specs = [
        pl.BlockSpec(
            (n_tp, 1, tile, features),
            lambda part, step, order_ref, block_ref, chunk_ref: (0, order_ref[part], step, 0),
        )
    ]
    in_specs += [fixed(value.shape) for value in (*weights, *far)]
    in_specs += [token_spec(index) for index in range(len(tokens))]
    in_specs += [pre, pre, fixed(gate_w.shape), fixed(up_w.shape)]
    operands = [cot, *weights, *far, *tokens, gate_pre, up_pre, gate_w, up_w]
    aliases = {3 + len(operands): 1, 4 + len(operands): 2}
    in_specs += [fixed(value.shape) for value in sums]
    operands += list(sums)
    return pl.pallas_call(
        functools.partial(
            chunk_kernel, len(tokens), len(weights) + 1, scale
        ),
        grid_spec=pltpu.PrefetchScalarGridSpec(
            num_scalar_prefetch=3,
            grid=(len(tokens), steps),
            in_specs=in_specs,
            out_specs=[
                pl.BlockSpec(
                    (1, tile, features),
                    lambda part, step, order_ref, block_ref, chunk_ref: (part, step, 0),
                ),
                fixed(gate_w.shape),
                fixed(up_w.shape),
            ],
        ),
        out_shape=[
            jax.ShapeDtypeStruct((len(tokens), rows, features), BF16),
            jax.ShapeDtypeStruct(gate_w.shape, F32),
            jax.ShapeDtypeStruct(up_w.shape, F32),
        ],
        input_output_aliases=aliases,
        name="chunk_grads",
    )(order, blocks, place, *operands)


def half_of(value, bit, keep):
    size = value.shape[0] // 2
    at = bit if keep else 1 - bit
    return lax.dynamic_slice_in_dim(value, at * size, size, 0)


def reduce_part(value, place, size, masks):
    for mask in masks:
        bit = (place // mask) % 2
        got = swap(half_of(value, bit, False).astype(BF16), "rep", size, mask)
        value = half_of(value, bit, True) + got.astype(F32)
    return value.astype(BF16)


def spread_part(piece, place, size, masks):
    pieces = {0: piece}
    for mask in reversed(masks):
        pieces.update({key ^ mask: swap(got, "rep", size, mask) for key, got in pieces.items()})
    offsets = {}
    for key in pieces:
        owner = place ^ key
        at = 0
        for mask in masks:
            at = at * 2 + (owner // mask) % 2
        offsets[key] = at
    return pieces, offsets


def place_kernel(n_pieces, start_ref, *refs):
    pieces, (out_ref, square_ref) = refs[:n_pieces], refs[n_pieces:]
    column = pl.program_id(0)

    @pl.when(column == 0)
    def _():
        square_ref[...] = jnp.zeros_like(square_ref)

    for index, ref in enumerate(pieces):
        rows = ref.shape[0]
        at = pl.ds(pl.multiple_of(start_ref[index] * rows, rows), rows)
        value = ref[...].astype(F32)
        out_ref[at, :] = value
        square_ref[at, :] += jnp.sum(value * value, axis=1, keepdims=True)


def place_rows(starts, pieces, rows):
    columns = pieces[0].shape[1]
    block = min(columns, 512)
    out, squares = pl.pallas_call(
        functools.partial(place_kernel, len(pieces)),
        grid_spec=pltpu.PrefetchScalarGridSpec(
            num_scalar_prefetch=1,
            grid=(columns // block,),
            in_specs=[
                pl.BlockSpec((piece.shape[0], block), lambda c, start_ref: (0, c))
                for piece in pieces
            ],
            out_specs=[
                pl.BlockSpec((rows, block), lambda c, start_ref: (0, c)),
                pl.BlockSpec((rows, 1), lambda c, start_ref: (0, 0)),
            ],
        ),
        out_shape=[
            jax.ShapeDtypeStruct((rows, columns), F32),
            jax.ShapeDtypeStruct((rows, 1), F32),
        ],
        name="place_rows",
    )(starts, *pieces)
    return out, squares[:, 0]


def sum_over_rep(value, place, size):
    masks = [1 << bit for bit in range(size.bit_length() - 1)]
    rows = value.shape[0]
    count = len(masks)
    part_rows = rows // count
    pieces, starts = [], []
    for index in range(count):
        turned = masks[index:] + masks[:index]
        part = value[index * part_rows:(index + 1) * part_rows]
        owned = reduce_part(part, place, size, turned)
        got, offsets = spread_part(owned, place, size, turned)
        for key in got:
            pieces.append(got[key])
            starts.append(index * size + offsets[key])
    starts = jnp.stack(starts).astype(jnp.int32)
    return place_rows(starts, pieces, rows)


def on_device(layer_input, cotangent, gate_pre, up_pre, gate_weight, up_weight, down_weight):
    n_rep, n_fs, n_tp = lax.axis_size("rep"), lax.axis_size("fs"), lax.axis_size("tp")
    rep, fs = lax.axis_index("rep"), lax.axis_index("fs")
    rows, features = cotangent.shape
    scale = 1.0 / math.sqrt(gate_pre.shape[0] * n_rep)
    order = ((fs + jnp.arange(n_fs)) % n_fs).astype(jnp.int32)
    tile = rows // TOKEN_CHUNKS

    share = down_weight.shape[0] // n_rep
    own = lax.all_gather(
        lax.dynamic_slice_in_dim(down_weight, rep * share, share, 0), "tp", axis=0
    )
    half = n_tp // 2
    near_x, near_y = swap(own, "rep", n_rep, 1), swap(own, "rep", n_rep, 2)
    far = (swap(near_x[:half], "rep", n_rep, 2), swap(near_y[half:], "rep", n_rep, 1))
    weights = (own, near_x, near_y)
    blocks = jnp.stack([rep, rep ^ 1, rep ^ 2, rep ^ 3]).astype(jnp.int32)

    chunks = [
        lax.all_gather(
            cotangent[index * tile:(index + 1) * tile], ("tp", "fs"), axis=0
        ).reshape(n_tp, n_fs, tile, features)
        for index in range(TOKEN_CHUNKS)
    ]

    cot_parts = [cotangent] + [rotate(cotangent, "fs", n_fs, k) for k in range(1, n_fs)]
    token_parts = [layer_input] + [rotate(layer_input, "fs", n_fs, k) for k in range(1, n_fs)]
    down_grad = down_partial(order, cot_parts, gate_pre, up_pre, scale, tile)
    down_grad, down_sq = sum_over_rep(down_grad, rep, n_rep)
    down_sq = lax.psum(down_sq, "tp")

    sums = (jnp.zeros(gate_weight.shape, F32), jnp.zeros(up_weight.shape, F32))
    kept, sent = [], []
    for index in range(TOKEN_CHUNKS):
        last = index == TOKEN_CHUNKS - 1
        if last:
            sums, down_sq = lax.optimization_barrier((sums, down_sq))
        partial, *sums = chunk_grads(
            order, blocks, chunks[index], weights, far, token_parts, gate_pre, up_pre,
            gate_weight, up_weight, sums, jnp.array([index, int(last)], jnp.int32), scale, tile,
        )
        kept.append(partial[0])
        sent.append(partial[1:])
    gate_grad, gate_sq = sum_over_rep(sums[0], rep, n_rep)
    up_grad, up_sq = sum_over_rep(sums[1], rep, n_rep)

    input_grad = jnp.concatenate(kept, 0).astype(F32)
    sent = jnp.concatenate(sent, 1)
    for k in range(1, n_fs):
        input_grad = input_grad + rotate(sent[k - 1], "fs", n_fs, -k).astype(F32)
    input_grad = input_grad.astype(BF16)
    gate_sq, up_sq = lax.psum((gate_sq, up_sq), "fs")
    return (input_grad, gate_grad, up_grad, down_grad, gate_sq, up_sq, down_sq)


def solution(mesh):
    return jax.shard_map(
        on_device,
        mesh=mesh,
        in_specs=(
            P(("rep", "fs"), "tp"),
            P(("rep", "fs"), "tp"),
            P("rep", "fs"),
            P("rep", "fs"),
            P("tp", "fs"),
            P("tp", "fs"),
            P("fs", "tp"),
        ),
        out_specs=(
            P(("rep", "fs"), "tp"),
            P("tp", "fs"),
            P("tp", "fs"),
            P("fs", "tp"),
            P("tp"),
            P("tp"),
            P("fs"),
        ),
        check_vma=False,
    )
```
